32 devices in a mesh: grp: 2 (over x), sp: 4 (over y, core), tp: 4 (over z).
Axes of the slice: x: 2, y: 2, z: 4, core: 2. Of those that a mesh axis runs over, the one named last changes fastest.
Arguments:
- attention_queryset: bfloat16 [2048, 1024], P(('grp', 'sp'), 'tp'), parts along dimension 0, may hold values from -6 to 6
- attention_keyset: bfloat16 [2048, 1024], P(('grp', 'sp'), 'tp'), parts along dimension 0, may hold values from -6 to 6
- attention_valueset: bfloat16 [2048, 1024], P(('grp', 'sp'), 'tp'), parts along dimension 0, may hold values from -6 to 6
- readout_switch_preactivation: bfloat16 [2048, 1024], P(('grp', 'sp'), 'tp'), parts along dimension 0, may hold values from -6 to 6
- retention_prelinear_score: float32 [2048, 8], P(('grp', 'sp'), 'tp'), parts along dimension 0, may hold values from -6 to 6
- additional_attenuation: float32 [2048, 8], P(('grp', 'sp'), 'tp'), parts along dimension 0, may hold values from -1.9 to 0
- feature_retention_logscale: float32 [8], P('tp'), may hold values from -14 to -2.4
- strength_prelinear_score: float32 [2048, 8], P(('grp', 'sp'), 'tp'), parts along dimension 0, may hold values from -9 to 1
- channel_rescale_vector: bfloat16 [128], replicated, may hold values from 0.099609375 to 1.8984375
- final_projection_matrix: bfloat16 [1024, 2048], replicated, may hold values from -0.1875 to 0.1875
- skip_stream: bfloat16 [2048, 2048], P(('grp', 'sp', 'tp')), parts along dimension 0, may hold values from -6 to 6
- specialist_rescale_vector: bfloat16 [2048], replicated, may hold values from 0.099609375 to 1.8984375
- specialist_switch_matrix: bfloat16 [16, 2048, 512], P(('sp', 'tp')), may hold values from -0.125 to 0.125
- specialist_widen_matrix: bfloat16 [16, 2048, 512], P(('sp', 'tp')), may hold values from -0.125 to 0.125
- specialist_contract_matrix: bfloat16 [16, 512, 2048], P(('sp', 'tp')), may hold values from -0.25 to 0.25
- chosen_specialist_ids: int32 [2048, 4], P(('grp', 'sp', 'tp')), parts along dimension 0, may hold values from 0 to 15, all different within a row; in each aligned block of 64 rows (0 to 63, 64 to 127, ...) at most 32 rows name the same one
- dispatch_shares: float32 [2048, 4], P(('grp', 'sp', 'tp')), parts along dimension 0, may hold values from 0.2 to 1.2
Outputs:
- output: bfloat16 [2048, 2048], P(('grp', 'sp', 'tp')), parts along dimension 0
The draws below stay inside these ranges and needn't reach their ends.
There are 2 independent parts, one for each index of `grp`. The reference program is written for one: setup_inputs(seed, part) draws one part's arguments, and reference() takes and returns one part's arrays. A program takes and returns all parts, laid end to end along the dimension named above; an argument that names none is the same for every part. Nothing has to cross between parts.
Inputs may be any that keep to these rules, and one draw needn't show every extreme that they name: `chosen_specialist_ids`: each row names 4 different experts; among the rows of one device no expert is named more than 32 times, a bound that some block reaches.
All inputs are finite; a program needn't handle non-finite values.
Results may differ from the reference program's by a relative error of at most 0.018.
Values may be sent and summed in bfloat16 or wider, within the bound.
A program may use at most 64 MiB of HBM per device.

```python
import math
import jax
import jax.numpy as jnp
import numpy as np
from jax import lax

D = 2048
HEADS = 8
HK = 128
FE = 512
TOPK = 4
BLK = 64
TOK_SP = 256
TOK_DEV = 64
TOKENS = 1024
EXPERTS = 16
CAP = 32


def draw_retention_prelinear_score(key, part):
    base = jax.random.normal(jax.random.fold_in(key, 11), (TOKENS, HEADS), jnp.float32)
    shift = jax.random.uniform(jax.random.fold_in(key, 12), (TOKENS // TOK_SP, 1), jnp.float32, -1.5, 1.5)
    return jnp.clip(base + jnp.repeat(shift, TOK_SP, axis=0), -6.0, 6.0)


def draw_additional_attenuation(key, part):
    places = jax.random.randint(jax.random.fold_in(key, 13), (3, HEADS), 0, TOKENS)
    amount = jnp.log(jax.random.uniform(jax.random.fold_in(key, 14), (3, HEADS), jnp.float32, 0.55, 0.8))
    position = lax.broadcasted_iota(jnp.int32, (TOKENS, 3, HEADS), 0)
    hits = (position == places[None]).astype(jnp.float32)
    return jnp.sum(hits * amount[None], axis=1)


def draw_feature_retention_logscale(key, part):
    order = jax.random.permutation(jax.random.fold_in(key, 15), HEADS)
    quick = HEADS // 2
    slow_rate = jnp.log(jax.random.uniform(jax.random.fold_in(key, 16), (HEADS,), jnp.float32, 0.05, 0.25) / TOKENS)
    fast_rate = jnp.log(jax.random.uniform(jax.random.fold_in(key, 17), (HEADS,), jnp.float32, 1.0 / 25.0, 1.0 / 12.0))
    return jnp.where(order < quick, fast_rate, slow_rate)


def draw_strength_prelinear_score(key, part):
    base = jax.random.normal(jax.random.fold_in(key, 21), (TOKENS, HEADS), jnp.float32)
    shift = jax.random.uniform(jax.random.fold_in(key, 22), (TOKENS // TOK_SP, 1), jnp.float32, -4.5, -2.5)
    return jnp.clip(base + jnp.repeat(shift, TOK_SP, axis=0), -9.0, 1.0)


def block_scale(stream_key, extent, split, low, largest):
    def one(axis_at, blocks):
        heights = jax.random.uniform(jax.random.fold_in(jax.random.fold_in(stream_key, 6), axis_at), (blocks,), jnp.float32, low / len(split), largest / len(split))
        return jnp.repeat(jnp.exp(heights), extent[axis_at] // blocks).reshape((-1,) + (1,) * (len(extent) - axis_at - 1))

    factor_of = one(*split[0])
    for cut in split[1:]:
        factor_of = factor_of * one(*cut)
    return factor_of


def deal_out(own_key, own, number, rows, number_of, top, reach, skew):
    sequence = jax.random.permutation(own_key, number_of)
    crowded, usual = portions_of(number_of, rows * top, reach, skew, True), portions_of(number_of, rows * top, reach, skew, False)
    places = jnp.arange(number_of)

    def named(sizes, offset_by):
        used = int((sizes > 0).sum())
        fixed = max(1, used // 4)
        moved = fixed + (places - fixed + offset_by * (used - fixed)) % max(1, number_of - fixed)
        return jnp.zeros((number_of,), jnp.int32).at[sequence[jnp.where(places < fixed, places, moved)]].set(jnp.asarray(sizes, jnp.int32))

    sizes = jnp.where(number % 4 == 0, named(crowded, number // 4), named(usual, number - number // 4 - 1))
    mixed = jax.random.permutation(jax.random.fold_in(own, 3), number_of)
    donor, receiver = mixed[0:number_of // 2 * 2:2], mixed[1:number_of // 2 * 2:2]
    room = jnp.minimum(sizes[donor] - 1, reach - sizes[receiver]) // 2
    room = jnp.where((donor == sequence[0]) | (receiver == sequence[0]) | (sizes[receiver] == 0), 0, jnp.maximum(room, 0))
    moved = jax.random.randint(jax.random.fold_in(own, 4), (number_of // 2,), 0, 1 << 20) % (room + 1)
    sizes = sizes.at[donor].add(-moved).at[receiver].add(moved)
    items = jnp.searchsorted(jnp.cumsum(sizes), jnp.arange(rows * top), side="right").astype(jnp.int32)
    listing = items.reshape(top, rows).T
    listing = listing[jax.random.permutation(jax.random.fold_in(own, 1), rows)]
    offset_by = jax.random.randint(jax.random.fold_in(own, 2), (rows, 1), 0, top)
    return jnp.take_along_axis(listing, (jnp.arange(top)[None, :] + offset_by) % top, axis=1)


def portions_of(number_of, total, bound, skew, full):
    weights = [(1 << 20) // math.isqrt(standing ** skew) + 1 for standing in range(1, number_of + 1)]
    largest = bound if full else min(bound, max(-(-total // number_of), total * weights[0] // sum(weights)))
    least = 1 if total - largest >= number_of - 1 else 0
    given, spare = [largest] + [least] * (number_of - 1), total - largest - least * (number_of - 1)
    while spare > 0:
        movable = [i for i in range(1, number_of) if given[i] < largest] or [i for i in range(1, number_of) if given[i] < bound]
        whole, left = sum([weights[i] for i in movable]), spare
        for i in movable:
            extra = min(bound - given[i], max(1, left * weights[i] // whole), spare)
            given[i] = given[i] + extra
            spare = spare - extra
    return np.array(given)


def bell_draw(key, dims, scale, bound, shards=(), kind=jnp.bfloat16):
    values = jax.random.normal(key, dims, jnp.float32) * scale
    if len(shards) > 0:
        values = block_scale(key, dims, shards, -0.22, 0.18) * values
    return jnp.clip(values, min=-bound, max=bound).astype(kind)


def setup_inputs(seed: int = 0, part: int = 0) -> dict:
    streams_of = jax.random.split(jax.random.key(seed), 18)
    part_keys = jax.random.split(jax.random.fold_in(streams_of[17], part), 18)
    attention_queryset = bell_draw(part_keys[0], (TOKENS, HEADS * HK), 1.0, 6.0, ((0, 4), (1, 4)))
    attention_keyset = bell_draw(part_keys[1], (TOKENS, HEADS * HK), 1.0, 6.0, ((0, 4), (1, 4)))
    attention_valueset = bell_draw(part_keys[2], (TOKENS, HEADS * HK), 1.0, 6.0, ((0, 4), (1, 4)))
    readout_switch_preactivation = bell_draw(part_keys[3], (TOKENS, HEADS * HK), 1.0, 6.0, ((0, 4), (1, 4)))
    retention_prelinear_score = draw_retention_prelinear_score(jax.random.fold_in(jax.random.fold_in(streams_of[17], part), 71), part)
    additional_attenuation = draw_additional_attenuation(jax.random.fold_in(jax.random.fold_in(streams_of[17], part), 71), part)
    feature_retention_logscale = draw_feature_retention_logscale(jax.random.fold_in(streams_of[17], 71), part)
    strength_prelinear_score = draw_strength_prelinear_score(jax.random.fold_in(jax.random.fold_in(streams_of[17], part), 71), part)
    channel_rescale_vector = jnp.clip(1.0 + 0.18 * jax.random.normal(streams_of[8], (HK,), jnp.float32), 0.099609375, 1.8984375).astype(jnp.bfloat16)
    final_projection_matrix = bell_draw(streams_of[9], (HEADS * HK, D), (HEADS * HK) ** -0.5, 0.1875)
    skip_stream = bell_draw(part_keys[10], (TOKENS, D), 1.0, 6.0, ((0, 16),))
    specialist_rescale_vector = jnp.clip(1.0 + 0.18 * jax.random.normal(streams_of[11], (D,), jnp.float32), 0.099609375, 1.8984375).astype(jnp.bfloat16)
    specialist_switch_matrix = bell_draw(streams_of[12], (EXPERTS, D, FE), D ** -0.5, 0.125, ((0, 16),))
    specialist_widen_matrix = bell_draw(streams_of[13], (EXPERTS, D, FE), D ** -0.5, 0.125, ((0, 16),))
    specialist_contract_matrix = bell_draw(streams_of[14], (EXPERTS, FE, D), FE ** -0.5, 0.25, ((0, 16),))
    chosen_specialist_ids_keys = jax.random.split(jax.random.fold_in(part_keys[15], 1), TOKENS // TOK_DEV)
    chosen_specialist_ids_turns = jax.random.permutation(jax.random.fold_in(part_keys[15], 3), TOKENS // TOK_DEV)
    chosen_specialist_ids = jax.vmap(lambda own, number: deal_out(jax.random.fold_in(part_keys[15], 2), own, number, TOK_DEV, EXPERTS, TOPK, CAP, 1))(chosen_specialist_ids_keys, chosen_specialist_ids_turns).reshape((TOKENS, TOPK))
    dispatch_shares = jnp.clip(0.2 + 1 * jax.random.uniform(part_keys[16], (TOKENS, TOPK), jnp.float32) ** block_scale(part_keys[16], (TOKENS, TOPK), ((0, 16),), -0.2, 0.2), 0.2, 1.2)
    return dict(attention_queryset=attention_queryset, attention_keyset=attention_keyset, attention_valueset=attention_valueset, readout_switch_preactivation=readout_switch_preactivation, retention_prelinear_score=retention_prelinear_score, additional_attenuation=additional_attenuation, feature_retention_logscale=feature_retention_logscale, strength_prelinear_score=strength_prelinear_score, channel_rescale_vector=channel_rescale_vector, final_projection_matrix=final_projection_matrix, skip_stream=skip_stream, specialist_rescale_vector=specialist_rescale_vector, specialist_switch_matrix=specialist_switch_matrix, specialist_widen_matrix=specialist_widen_matrix, specialist_contract_matrix=specialist_contract_matrix, chosen_specialist_ids=chosen_specialist_ids, dispatch_shares=dispatch_shares)


epsilon = 1e-06
exact_mode = lax.Precision.HIGHEST

def unit_rows(array):
    floats = array.astype(jnp.float32)
    return floats * lax.rsqrt(lax.optimization_barrier(jnp.sum(floats * floats, axis=-1, keepdims=True)) + epsilon)

def to_blocks(array, count, length):
    return jnp.moveaxis(array.reshape((count, length) + array.shape[1:]), 2, 0)

def block_terms(query_blk, key_blk, value_blk, log_cum, strength):
    length = query_blk.shape[2]
    row_pos = lax.broadcasted_iota(jnp.int32, (length, length), 0)
    col_pos = lax.broadcasted_iota(jnp.int32, (length, length), 1)
    causal = row_pos >= col_pos
    spread = log_cum[..., :, None] - log_cum[..., None, :]
    decay = jnp.where(causal, jnp.exp(jnp.where(causal, spread, 0.0)), 0.0)
    key_key = jnp.einsum('hnid,hnjd->hnij', key_blk, key_blk, precision=exact_mode)
    lower = jnp.where(row_pos > col_pos, strength[..., :, None] * key_key * decay, 0.0)
    system = jnp.eye(length, dtype=jnp.float32) + lower
    right = jnp.concatenate([value_blk * strength[..., None], key_blk * (strength * jnp.exp(log_cum))[..., None]], axis=-1)
    solved = jax.scipy.linalg.solve_triangular(system, right, lower=True, unit_diagonal=True)
    width = value_blk.shape[-1]
    fixed_values = solved[..., :width]
    fixed_keys = solved[..., width:]
    query_key = jnp.einsum('hnid,hnjd->hnij', query_blk, key_blk, precision=exact_mode) * decay
    query_dec = query_blk * jnp.exp(log_cum)[..., None]
    key_dec = key_blk * jnp.exp(log_cum[..., -1:] - log_cum)[..., None]
    last_decay = jnp.exp(log_cum[..., -1])
    return (query_key, fixed_values, fixed_keys, query_dec, key_dec, last_decay)

def assemble_parameters(attention_queryset, attention_keyset, attention_valueset, retention_prelinear_score, additional_attenuation, feature_retention_logscale, strength_prelinear_score):
    tokens_here, heads = retention_prelinear_score.shape
    count = tokens_here // BLK
    query_all = unit_rows(attention_queryset.reshape(tokens_here, heads, HK)) * HK ** (-0.5)
    key_all = unit_rows(attention_keyset.reshape(tokens_here, heads, HK))
    value_all = attention_valueset.reshape(tokens_here, heads, HK).astype(jnp.float32)
    forgetting_exponent = -jnp.exp(feature_retention_logscale)[None, :] * jax.nn.softplus(retention_prelinear_score) + additional_attenuation
    log_cum = jnp.cumsum(to_blocks(forgetting_exponent, count, BLK), axis=-1)
    strength = jax.nn.sigmoid(to_blocks(strength_prelinear_score, count, BLK))
    return block_terms(to_blocks(query_all, count, BLK), to_blocks(key_all, count, BLK), to_blocks(value_all, count, BLK), log_cum, strength)

def project(left, right):
    return jnp.einsum('hcd,hde->hce', left, right, precision=exact_mode)

def propagate(state, fresh, key_dec, last_decay):
    return state * last_decay[:, None, None] + jnp.einsum('hcd,hce->hde', key_dec, fresh, precision=exact_mode)

def read_step(state, inputs):
    query_key, fixed_values, fixed_keys, query_dec, key_dec, last_decay = inputs
    fresh = fixed_values - project(fixed_keys, state)
    output = project(query_dec, state) + project(query_key, fresh)
    return (propagate(state, fresh, key_dec, last_decay), output)

def head_finish(outputs, readout_switch_preactivation, channel_rescale_vector):
    count, heads, length, width = outputs.shape
    flat = jnp.transpose(outputs, (0, 2, 1, 3)).reshape(count * length, heads, width)
    scaled = flat * lax.rsqrt(lax.optimization_barrier(jnp.mean(flat * flat, axis=-1, keepdims=True)) + epsilon)
    scaled = scaled * channel_rescale_vector.astype(jnp.float32)
    gate = readout_switch_preactivation.reshape(count * length, heads, width).astype(jnp.float32)
    return (scaled * jax.nn.silu(gate)).reshape(count * length, heads * width).astype(jnp.bfloat16)

def rms_gain(array, gain):
    floats = array.astype(jnp.float32)
    scaled = floats * lax.rsqrt(lax.optimization_barrier(jnp.mean(floats * floats, axis=-1, keepdims=True)) + epsilon)
    return (scaled * gain.astype(jnp.float32)).astype(jnp.bfloat16)

def expert_mlp(rows, gate_weight, up_weight, down_weight):
    gate = jnp.dot(rows.astype(jnp.float32), gate_weight.astype(jnp.float32), preferred_element_type=jnp.float32)
    upward = jnp.dot(rows.astype(jnp.float32), up_weight.astype(jnp.float32), preferred_element_type=jnp.float32)
    hidden = (jax.nn.silu(gate) * upward).astype(jnp.bfloat16)
    return jnp.dot(hidden.astype(jnp.float32), down_weight.astype(jnp.float32), preferred_element_type=jnp.float32).astype(jnp.bfloat16)

def reference(attention_queryset, attention_keyset, attention_valueset, readout_switch_preactivation, retention_prelinear_score, additional_attenuation, feature_retention_logscale, strength_prelinear_score, channel_rescale_vector, final_projection_matrix, skip_stream, specialist_rescale_vector, specialist_switch_matrix, specialist_widen_matrix, specialist_contract_matrix, chosen_specialist_ids, dispatch_shares):
    portion_increments = assemble_parameters(attention_queryset, attention_keyset, attention_valueset, retention_prelinear_score, additional_attenuation, feature_retention_logscale, strength_prelinear_score)
    piled_together = tuple((jnp.moveaxis(element_entry, 1, 0) for element_entry in portion_increments))
    start = jnp.zeros((HEADS, HK, HK), jnp.float32)
    _, outputs = lax.scan(read_step, start, piled_together)
    mixed = head_finish(outputs, readout_switch_preactivation, channel_rescale_vector)
    merged = (skip_stream.astype(jnp.float32) + jnp.dot(mixed.astype(jnp.float32), final_projection_matrix.astype(jnp.float32), preferred_element_type=jnp.float32)).astype(jnp.bfloat16)
    normed = rms_gain(merged, specialist_rescale_vector)
    limit = TOKENS // TOK_DEV * CAP
    flat_ids = chosen_specialist_ids.reshape(-1)
    flat_weights = dispatch_shares.reshape(-1)
    total = flat_ids.shape[0]

    def expert_step(index, summed):
        picked = jnp.nonzero(flat_ids == index, size=limit, fill_value=total)[0].astype(jnp.int32)
        valid = picked < total
        safe = jnp.minimum(picked, total - 1).astype(jnp.int32)
        token_index = (safe // TOPK).astype(jnp.int32)
        result = expert_mlp(normed[token_index], specialist_switch_matrix[index], specialist_widen_matrix[index], specialist_contract_matrix[index])
        weight = jnp.where(valid, flat_weights[safe], 0.0)
        return summed.at[token_index].add(weight[:, None] * result.astype(jnp.float32))
    summed = lax.fori_loop(0, EXPERTS, expert_step, jnp.zeros((TOKENS, D), jnp.float32))
    return (merged.astype(jnp.float32) + summed).astype(jnp.bfloat16)
```

```python
import functools

import jax
import jax.numpy as jnp
from jax import lax
from jax.experimental import pallas as pl
from jax.experimental.pallas import tpu as pltpu
from jax.sharding import PartitionSpec as P

HK = 128
epsilon = 1e-06
MESH = pl.DeviceIdType.MESH
VLIM = 64 * 1024 * 1024 - 128 * 1024


def split2(a):
    hi = a.astype(jnp.bfloat16)
    return hi, (a - hi.astype(jnp.float32)).astype(jnp.bfloat16)


def dims(ca, cb):
    return (((ca,), (cb,)), ((), ()))


def dot1(a, b, ca=1, cb=0):
    return lax.dot_general(a, b, dims(ca, cb), preferred_element_type=jnp.float32)


def dot3(a, b, ca=1, cb=0):
    return dot1(a[0], b[0], ca, cb) + (dot1(a[0], b[1], ca, cb) + dot1(a[1], b[0], ca, cb))


def attention_kernel(q_ref, k_ref, v_ref, ld_ref, st_ref, o_ref, qe_ref, m_ref, s_ref):
    length, heads = ld_ref.shape
    row = lax.broadcasted_iota(jnp.int32, (length, length), 0)
    col = lax.broadcasted_iota(jnp.int32, (length, length), 1)
    causal = row >= col
    strict = row > col
    tri = causal.astype(jnp.float32)
    ld = ld_ref[...]
    cum_col = lax.dot_general(tri, ld, dims(1, 0), precision=lax.Precision.HIGHEST,
                              preferred_element_type=jnp.float32)
    cum_row = lax.dot_general(ld, tri, dims(0, 1), precision=lax.Precision.HIGHEST,
                              preferred_element_type=jnp.float32)
    beta_all = jax.nn.sigmoid(st_ref[...])
    eye = (row == col).astype(jnp.float32)
    eye_k = (lax.broadcasted_iota(jnp.int32, (HK, HK), 0)
             == lax.broadcasted_iota(jnp.int32, (HK, HK), 1)).astype(jnp.float32)
    xs, lows, keep = [], [], []
    for h in range(heads):
        sl = slice(h * HK, (h + 1) * HK)
        q = q_ref[:, sl].astype(jnp.float32)
        k = k_ref[:, sl].astype(jnp.float32)
        v = v_ref[:, sl].astype(jnp.float32)
        q = q * lax.rsqrt(jnp.sum(q * q, axis=1, keepdims=True) + epsilon) * HK ** (-0.5)
        k = k * lax.rsqrt(jnp.sum(k * k, axis=1, keepdims=True) + epsilon)
        c = cum_col[:, h:h + 1]
        r = cum_row[h:h + 1, :]
        beta = beta_all[:, h:h + 1]
        decay = jnp.where(causal, jnp.exp(jnp.minimum(c - r, 0.0)), 0.0)
        ks = split2(k)
        lower = jnp.where(strict, beta * dot3(ks, ks, 1, 1) * decay, 0.0)
        scores = split2(dot3(split2(q), ks, 1, 1) * decay)
        lows.append(lower)
        keep.append((q, k, v, c, beta, scores))
        n = jnp.where((row // 8) == (col // 8), -lower, 0.0)
        n1 = split2(n)
        n2f = dot3(n1, n1)
        n2 = split2(n2f)
        p = eye + n
        p = p + dot3(split2(p), n2)
        n4 = split2(dot3(n2, n2))
        xs.append(p + dot3(split2(p), n4))
    size = 8
    while size < length:
        mask = ((row // (2 * size)) == (col // (2 * size))) & ((row // size) != (col // size))
        for h in range(heads):
            part = split2(jnp.where(mask, lows[h], 0.0))
            x2 = split2(xs[h])
            xs[h] = xs[h] - dot3(x2, split2(dot3(part, x2)))
        size *= 2
    for h in range(heads):
        sl = slice(h * HK, (h + 1) * HK)
        q, k, v, c, beta, scores = keep[h]
        up = jnp.exp(c)
        last = c[length - 1:length, :]
        right = jnp.concatenate([v * beta, k * (beta * up)], axis=1)
        uw = split2(dot3(split2(xs[h]), split2(right)))
        mixed = dot3(scores, uw)
        o_ref[:, sl] = mixed[:, :HK]
        qe_ref[:, sl] = q * up - mixed[:, HK:]
        ends = dot3(split2(k * jnp.exp(last - c)), uw, 0, 0)
        s_ref[h] = ends[:, :HK]
        m_ref[h] = jnp.exp(last) * eye_k - ends[:, HK:]


def attention_terms(q, k, v, log_decay, strength_pre):
    length, heads = log_decay.shape
    f32 = jnp.float32
    vm = pl.BlockSpec(memory_space=pltpu.VMEM)
    return pl.pallas_call(
        attention_kernel,
        out_shape=(
            jax.ShapeDtypeStruct((length, heads * HK), f32),
            jax.ShapeDtypeStruct((length, heads * HK), f32),
            jax.ShapeDtypeStruct((heads, HK, HK), f32),
            jax.ShapeDtypeStruct((heads, HK, HK), f32),
        ),
        in_specs=[vm] * 5,
        out_specs=(vm,) * 4,
        compiler_params=pltpu.CompilerParams(vmem_limit_bytes=32 * 1024 * 1024),
        name="attention_terms",
    )(q, k, v, log_decay, strength_pre)


def experts_kernel(ny, nz, rows, width, experts, x_ref, merged_ref, wg_hbm, wu_hbm, wd_hbm, out_ref,
                   G, Pt, CR, YR, ZR, wg, wu, wd, wsem, own_sem,
                   zs, zr, ys, yr, cs, cr, rcs, rcr, rys, ryr, rzs, rzr):
    sp = lax.axis_index("sp")
    z = lax.axis_index("tp")
    y = sp // 2
    c = sp % 2
    pc = 1 - c
    me = sp * nz + z
    expert = me
    f32 = jnp.float32

    def slot(yy, cc, zz):
        return (yy * 2 + cc) * nz + zz

    loads = [pltpu.make_async_copy(s, d, wsem.at[i])
             for i, (s, d) in enumerate(((wg_hbm, wg), (wu_hbm, wu), (wd_hbm, wd)))]
    for load in loads:
        load.start()
    own = pltpu.make_async_copy(x_ref, G.at[me], own_sem)
    own.start()

    barrier = pltpu.get_barrier_semaphore()
    greet = [{"tp": lax.rem(z + 1, nz)}, {"tp": lax.rem(z + nz - 1, nz)},
             {"sp": lax.rem(y + 1, ny) * 2 + c}, {"sp": lax.rem(y + ny - 1, ny) * 2 + c},
             {"sp": y * 2 + pc}]
    for d in greet:
        pl.semaphore_signal(barrier, inc=1, device_id=d, device_id_type=MESH)
    pl.semaphore_wait(barrier, len(greet))

    def remote(src, dst, ssem, rsem, dev):
        return pltpu.make_async_remote_copy(src_ref=src, dst_ref=dst, send_sem=ssem, recv_sem=rsem,
                                            device_id=dev, device_id_type=MESH)

    def z_copy(d, b, src=None):
        sl = slot(y, c, b)
        return remote(G.at[sl] if src is None else src, G.at[sl], zs.at[d, b], zr.at[b],
                      {"tp": z + (1 if d == 0 else -1)})

    def y_copy(d, yy, b, src=None):
        sl = slot(yy, c, b)
        return remote(G.at[sl] if src is None else src, G.at[sl], ys.at[d, yy, b], yr.at[yy, b],
                      {"sp": (y + (1 if d == 0 else -1)) * 2 + c})

    def c_copy(yy, b, cc=None, src=None):
        cc = c if cc is None else cc
        sl = slot(yy, cc, b)
        return remote(G.at[sl] if src is None else src, G.at[sl], cs.at[yy, b], cr.at[yy, b],
                      {"sp": y * 2 + pc})

    def fan_y(b, src=None):
        @pl.when(y + 1 < ny)
        def _():
            y_copy(0, y, b, src).start()

        @pl.when(y > 0)
        def _():
            y_copy(1, y, b, src).start()

    @pl.when(z + 1 < nz)
    def _():
        z_copy(0, z, x_ref).start()

    @pl.when(z > 0)
    def _():
        z_copy(1, z, x_ref).start()

    fan_y(z, x_ref)
    c_copy(y, z, src=x_ref).start()
    own.wait()

    @pl.loop(1, nz)
    def _(s):
        for d in (0, 1):
            b = z - s if d == 0 else z + s
            ok = b >= 0 if d == 0 else b < nz
            onward = z + 1 < nz if d == 0 else z > 0

            @pl.when(ok)
            def _():
                z_copy(d, b).wait_recv()

                @pl.when(onward)
                def _():
                    z_copy(d, b).start()

                fan_y(b)
                c_copy(y, b).start()

    def compute(yy, cc):
        first = slot(yy, cc, 0)
        x = jnp.concatenate([G[first + b, :, :width] for b in range(nz)], axis=0)
        tail = jnp.concatenate([G[first + b, :, width:] for b in range(nz)], axis=0).astype(f32)
        lane = lax.broadcasted_iota(jnp.int32, tail.shape, 1)
        share = jnp.sum(jnp.where((lane == expert) | (lane == expert + experts), tail, 0.0),
                        axis=1, keepdims=True)
        gate = jnp.dot(x, wg[...], preferred_element_type=f32)
        upward = jnp.dot(x, wu[...], preferred_element_type=f32)
        hidden = (jax.nn.silu(gate) * upward).astype(jnp.bfloat16)
        half = width // 2
        for i in range(2):
            cols = slice(i * half, (i + 1) * half)
            got = (jnp.dot(hidden, wd[:, cols], preferred_element_type=f32) * share).astype(jnp.bfloat16)
            for b in range(nz):
                Pt[first + b, :, cols] = got[b * rows:(b + 1) * rows]

    for load in loads:
        load.wait()

    @pl.loop(1, ny)
    def _(t):
        for d in (0, 1):
            yy = y - t if d == 0 else y + t
            ok = yy >= 0 if d == 0 else yy < ny
            onward = y + 1 < ny if d == 0 else y > 0

            @pl.when(ok)
            def _():
                @pl.loop(0, nz)
                def _(b):
                    y_copy(d, yy, b).wait_recv()

                    @pl.when(onward)
                    def _():
                        y_copy(d, yy, b).start()

                    c_copy(yy, b).start()

    def rc_copy(yy, b):
        return remote(Pt.at[slot(yy, pc, b)], CR.at[yy, b], rcs.at[yy, b], rcr.at[yy, b],
                      {"sp": y * 2 + pc})

    @pl.loop(0, 2 * ny)
    def _(j):
        yy = lax.rem(y + lax.rem(j, ny), ny)
        cc = jnp.where(j < ny, pc, c)

        @pl.when(j < ny)
        def _():
            @pl.loop(0, nz)
            def _(b):
                c_copy(yy, b, cc=pc).wait_recv()

        compute(yy, cc)

        @pl.when(j < ny)
        def _():
            @pl.loop(0, nz)
            def _(b):
                rc_copy(yy, b).start()

    def add_to(sl, other):
        Pt[sl] = (Pt[sl].astype(f32) + other.astype(f32)).astype(jnp.bfloat16)

    def ry_copy(d, yy, b):
        dest = y + (1 if d == 0 else -1)
        place = yy if d == 0 else jnp.where(yy == dest, ny, yy)
        return remote(Pt.at[slot(yy, c, b)], YR.at[place, b], rys.at[d, yy, b], ryr.at[place, b],
                      {"sp": dest * 2 + c})

    def ry_wait(place, b):
        remote(YR.at[place, b], YR.at[place, b], rys.at[0, 0, b], ryr.at[place, b],
               {"sp": y * 2 + pc}).wait_recv()

    @pl.loop(0, ny - 1)
    def _(t):
        for d in (0, 1):
            yy = ny - 1 - t if d == 0 else t
            ok = yy > y if d == 0 else yy < y
            behind = y > 0 if d == 0 else y + 1 < ny

            @pl.when(ok)
            def _():
                @pl.loop(0, nz)
                def _(i):
                    b = jnp.where(lax.rem(i, 2) == 0, nz - 1 - i // 2, i // 2)
                    sl = slot(yy, c, b)
                    rc_copy(yy, b).wait_recv()
                    add_to(sl, CR[yy, b])

                    @pl.when(behind)
                    def _():
                        ry_wait(yy, b)
                        add_to(sl, YR[yy, b])

                    ry_copy(d, yy, b).start()

    def rz_copy(d, b):
        dest = z + (1 if d == 0 else -1)
        place = b if d == 0 else jnp.where(b == dest, nz, b)
        return remote(Pt.at[slot(y, c, b)], ZR.at[place], rzs.at[d, b], rzr.at[place], {"tp": dest})

    def rz_wait(place):
        remote(ZR.at[place], ZR.at[place], rzs.at[0, 0], rzr.at[place], {"tp": z}).wait_recv()

    @pl.loop(0, nz)
    def _(i):
        b = jnp.where(lax.rem(i, 2) == 0, nz - 1 - i // 2, i // 2)
        sl = slot(y, c, b)
        rc_copy(y, b).wait_recv()
        add_to(sl, CR[y, b])

        @pl.when(y > 0)
        def _():
            ry_wait(y, b)
            add_to(sl, YR[y, b])

        @pl.when(y + 1 < ny)
        def _():
            ry_wait(ny, b)
            add_to(sl, YR[ny, b])

        for d in (0, 1):
            ok = b > z if d == 0 else b < z
            behind = z > 0 if d == 0 else z + 1 < nz

            @pl.when(ok)
            def _():
                @pl.when(behind)
                def _():
                    rz_wait(b)
                    add_to(sl, ZR[b])

                rz_copy(d, b).start()

    @pl.when(z > 0)
    def _():
        rz_wait(z)
        add_to(me, ZR[z])

    @pl.when(z + 1 < nz)
    def _():
        rz_wait(nz)
        add_to(me, ZR[nz])

    out_ref[...] = (merged_ref[...].astype(f32) + Pt[me].astype(f32)).astype(jnp.bfloat16)

    @pl.loop(0, nz)
    def _(b):
        @pl.when((z + 1 < nz) & (b <= z))
        def _():
            z_copy(0, b).wait_send()

        @pl.when((z > 0) & (b >= z))
        def _():
            z_copy(1, b).wait_send()

        @pl.when(b > z)
        def _():
            rz_copy(0, b).wait_send()

        @pl.when(b < z)
        def _():
            rz_copy(1, b).wait_send()

        @pl.loop(0, ny)
        def _(yy):
            c_copy(yy, b).wait_send()
            rc_copy(yy, b).wait_send()

            @pl.when((y + 1 < ny) & (yy <= y))
            def _():
                y_copy(0, yy, b).wait_send()

            @pl.when((y > 0) & (yy >= y))
            def _():
                y_copy(1, yy, b).wait_send()

            @pl.when(yy > y)
            def _():
                ry_copy(0, yy, b).wait_send()

            @pl.when(yy < y)
            def _():
                ry_copy(1, yy, b).wait_send()


def run_experts(payload, merged, wg, wu, wd, ny, nz, experts):
    rows, width = merged.shape
    wide = payload.shape[1]
    hidden = wg.shape[1]
    blocks = ny * 2 * nz
    bf = jnp.bfloat16
    vm = pl.BlockSpec(memory_space=pltpu.VMEM)
    hbm = pl.BlockSpec(memory_space=pl.ANY)
    dma = pltpu.SemaphoreType.DMA
    return pl.pallas_call(
        functools.partial(experts_kernel, ny, nz, rows, width, experts),
        out_shape=jax.ShapeDtypeStruct((rows, width), bf),
        in_specs=[vm, vm, hbm, hbm, hbm],
        out_specs=vm,
        scratch_shapes=[
            pltpu.VMEM((blocks, rows, wide), bf),
            pltpu.VMEM((blocks, rows, width), bf),
            pltpu.VMEM((ny, nz, rows, width), bf),
            pltpu.VMEM((ny + 1, nz, rows, width), bf),
            pltpu.VMEM((nz + 1, rows, width), bf),
            pltpu.VMEM((width, hidden), bf),
            pltpu.VMEM((width, hidden), bf),
            pltpu.VMEM((hidden, width), bf),
            dma((3,)), dma,
            dma((2, nz)), dma((nz,)),
            dma((2, ny, nz)), dma((ny, nz)),
            dma((ny, nz)), dma((ny, nz)),
            dma((ny, nz)), dma((ny, nz)),
            dma((2, ny, nz)), dma((ny + 1, nz)),
            dma((2, nz)), dma((nz + 1,)),
        ],
        compiler_params=pltpu.CompilerParams(
            collective_id=3, has_side_effects=True, vmem_limit_bytes=VLIM),
        name="routed_experts",
    )(payload, merged, wg, wu, wd)


def prefix_state(m, s, axis):
    place = lax.axis_index(axis)
    ms = lax.all_gather(jnp.concatenate([m, s], axis=-1), axis)

    def one(hop, state):
        got = lax.dynamic_index_in_dim(ms, hop, 0, False)
        return jnp.einsum("hcd,hde->hce", got[..., :HK], state, precision=lax.Precision.HIGHEST) + got[..., HK:]

    return lax.fori_loop(0, place, one, jnp.zeros_like(s))


def local(
    attention_queryset,
    attention_keyset,
    attention_valueset,
    readout_switch_preactivation,
    retention_prelinear_score,
    additional_attenuation,
    feature_retention_logscale,
    strength_prelinear_score,
    channel_rescale_vector,
    final_projection_matrix,
    skip_stream,
    specialist_rescale_vector,
    specialist_switch_matrix,
    specialist_widen_matrix,
    specialist_contract_matrix,
    chosen_specialist_ids,
    dispatch_shares,
):
    f32 = jnp.float32
    bf = jnp.bfloat16
    tokens, heads = retention_prelinear_score.shape
    nsp = lax.axis_size("sp")
    nz = lax.axis_size("tp")
    ny = nsp // 2
    experts = nsp * nz
    log_decay = (
        -jnp.exp(feature_retention_logscale)[None, :] * jax.nn.softplus(retention_prelinear_score)
        + additional_attenuation
    )
    o, qe, m, s = attention_terms(
        attention_queryset, attention_keyset, attention_valueset, log_decay, strength_prelinear_score)
    start = prefix_state(m, s, "sp")
    out = o.reshape(tokens, heads, HK) + jnp.einsum(
        "thd,hde->the", qe.reshape(tokens, heads, HK), start, precision=lax.Precision.HIGHEST)
    scaled = out * lax.rsqrt(jnp.mean(out * out, axis=-1, keepdims=True) + epsilon)
    scaled = scaled * channel_rescale_vector.astype(f32)
    gate = readout_switch_preactivation.reshape(tokens, heads, HK).astype(f32)
    mixed = (scaled * jax.nn.silu(gate)).reshape(tokens, heads * HK).astype(bf)
    own_rows = lax.all_to_all(mixed, "tp", split_axis=0, concat_axis=1, tiled=True)
    merged = (
        skip_stream.astype(f32)
        + jnp.dot(own_rows, final_projection_matrix, preferred_element_type=f32)
    ).astype(bf)
    floats = merged.astype(f32)
    normed = (floats * lax.rsqrt(jnp.mean(floats * floats, axis=-1, keepdims=True) + epsilon)
              * specialist_rescale_vector.astype(f32)).astype(bf)
    rows = normed.shape[0]
    lanes = -(-2 * experts // 128) * 128
    lane = lax.broadcasted_iota(jnp.int32, (rows, lanes), 1)
    tail = jnp.zeros((rows, lanes), f32)
    for i in range(chosen_specialist_ids.shape[1]):
        share = dispatch_shares[:, i:i + 1]
        high = share.astype(bf).astype(f32)
        chosen = chosen_specialist_ids[:, i:i + 1]
        tail = tail + jnp.where(lane == chosen, high, 0.0)
        tail = tail + jnp.where(lane == chosen + experts, share - high, 0.0)
    payload = jnp.concatenate([normed, tail.astype(bf)], axis=1)
    return run_experts(payload, merged, specialist_switch_matrix[0], specialist_widen_matrix[0],
                       specialist_contract_matrix[0], ny, nz, experts)


def solution(mesh):
    return jax.shard_map(
        local,
        mesh=mesh,
        in_specs=(
            P(("grp", "sp"), "tp"),
            P(("grp", "sp"), "tp"),
            P(("grp", "sp"), "tp"),
            P(("grp", "sp"), "tp"),
            P(("grp", "sp"), "tp"),
            P(("grp", "sp"), "tp"),
            P("tp"),
            P(("grp", "sp"), "tp"),
            P(),
            P(),
            P(("grp", "sp", "tp"), None),
            P(),
            P(("sp", "tp"), None, None),
            P(("sp", "tp"), None, None),
            P(("sp", "tp"), None, None),
            P(("grp", "sp", "tp"), None),
            P(("grp", "sp", "tp"), None),
        ),
        out_specs=P(("grp", "sp", "tp"), None),
        check_vma=False,
    )
```

```python
import functools

import jax
import jax.numpy as jnp
from jax import lax
from jax.experimental import pallas as pl
from jax.experimental.pallas import tpu as pltpu
from jax.sharding import PartitionSpec as P

HK = 128
epsilon = 1e-06
MESH = pl.DeviceIdType.MESH
VLIM = 64 * 1024 * 1024 - 128 * 1024


def split2(a):
    hi = a.astype(jnp.bfloat16)
    return hi, (a - hi.astype(jnp.float32)).astype(jnp.bfloat16)


def dims(ca, cb):
    return (((ca,), (cb,)), ((), ()))


def dot1(a, b, ca=1, cb=0):
    return lax.dot_general(a, b, dims(ca, cb), preferred_element_type=jnp.float32)


def dot3(a, b, ca=1, cb=0):
    return dot1(a[0], b[0], ca, cb) + (dot1(a[0], b[1], ca, cb) + dot1(a[1], b[0], ca, cb))


def attention_kernel(q_ref, k_ref, v_ref, g_ref, sc_ref, ad_ref, ls_ref, st_ref, gain_ref, wo_hbm, skip_ref,
                     rescale_ref, ids_ref, share_ref, pay_ref, merged_ref,
                     o_ref, qe_ref, m_ref, s_ref, start_ref, next_ref, mixed_ref, own_ref, wo,
                     wsem, chain_s, chain_r, swap_s, swap_r):
    heads, length = sc_ref.shape
    f32 = jnp.float32
    sp = lax.axis_index("sp")
    z = lax.axis_index("tp")
    nsp = lax.axis_size("sp")
    nz = lax.axis_size("tp")
    rows, width = merged_ref.shape
    load = pltpu.make_async_copy(wo_hbm, wo, wsem)
    load.start()
    barrier = pltpu.get_barrier_semaphore()
    greet = [{"sp": lax.rem(sp + 1, nsp)}, {"sp": lax.rem(sp + nsp - 1, nsp)}]
    greet += [{"tp": lax.rem(z + d, nz)} for d in range(1, nz)]
    for d in greet:
        pl.semaphore_signal(barrier, inc=1, device_id=d, device_id_type=MESH)
    row = lax.broadcasted_iota(jnp.int32, (length, length), 0)
    col = lax.broadcasted_iota(jnp.int32, (length, length), 1)
    causal = row >= col
    strict = row > col
    tri = causal.astype(jnp.float32)
    score = sc_ref[...]
    soft = jnp.maximum(score, 0.0) + jnp.log1p(jnp.exp(-jnp.abs(score)))
    ld = ad_ref[...] - jnp.exp(ls_ref[...]) * soft
    cum_col = lax.dot_general(tri, ld, dims(1, 1), precision=lax.Precision.HIGHEST,
                              preferred_element_type=jnp.float32)
    cum_row = lax.dot_general(ld, tri, dims(1, 1), precision=lax.Precision.HIGHEST,
                              preferred_element_type=jnp.float32)
    eye = (row == col).astype(jnp.float32)
    beta_all = lax.dot_general(eye, jax.nn.sigmoid(st_ref[...]), dims(1, 1), precision=lax.Precision.HIGHEST,
                               preferred_element_type=jnp.float32)
    eye_k = (lax.broadcasted_iota(jnp.int32, (HK, HK), 0)
             == lax.broadcasted_iota(jnp.int32, (HK, HK), 1)).astype(jnp.float32)
    xs, lows, keep = [], [], []
    for h in range(heads):
        sl = slice(h * HK, (h + 1) * HK)
        q = q_ref[:, sl].astype(jnp.float32)
        k = k_ref[:, sl].astype(jnp.float32)
        v = v_ref[:, sl].astype(jnp.float32)
        q = q * lax.rsqrt(jnp.sum(q * q, axis=1, keepdims=True) + epsilon) * HK ** (-0.5)
        k = k * lax.rsqrt(jnp.sum(k * k, axis=1, keepdims=True) + epsilon)
        c = cum_col[:, h:h + 1]
        r = cum_row[h:h + 1, :]
        beta = beta_all[:, h:h + 1]
        decay = jnp.where(causal, jnp.exp(jnp.minimum(c - r, 0.0)), 0.0)
        ks = split2(k)
        lower = jnp.where(strict, beta * dot3(ks, ks, 1, 1) * decay, 0.0)
        scores = split2(dot3(split2(q), ks, 1, 1) * decay)
        lows.append(lower)
        keep.append((q, k, v, c, beta, scores))
        n = jnp.where((row // 8) == (col // 8), -lower, 0.0)
        n1 = split2(n)
        n2f = dot3(n1, n1)
        n2 = split2(n2f)
        p = eye + n
        p = p + dot3(split2(p), n2)
        n4 = split2(dot3(n2, n2))
        xs.append(p + dot3(split2(p), n4))
    size = 8
    while size < length:
        mask = ((row // (2 * size)) == (col // (2 * size))) & ((row // size) != (col // size))
        for h in range(heads):
            part = split2(jnp.where(mask, lows[h], 0.0))
            x2 = split2(xs[h])
            xs[h] = xs[h] - dot3(x2, split2(dot3(part, x2)))
        size *= 2
    for h in range(heads):
        sl = slice(h * HK, (h + 1) * HK)
        q, k, v, c, beta, scores = keep[h]
        up = jnp.exp(c)
        last = c[length - 1:length, :]
        right = jnp.concatenate([v * beta, k * (beta * up)], axis=1)
        uw = split2(dot3(split2(xs[h]), split2(right)))
        mixed = dot3(scores, uw)
        o_ref[:, sl] = mixed[:, :HK]
        qe_ref[:, sl] = q * up - mixed[:, HK:]
        ends = dot3(split2(k * jnp.exp(last - c)), uw, 0, 0)
        s_ref[h] = ends[:, :HK]
        m_ref[h] = jnp.exp(last) * eye_k - ends[:, HK:]

    pl.semaphore_wait(barrier, len(greet))

    def pass_on(to):
        return pltpu.make_async_remote_copy(src_ref=next_ref, dst_ref=start_ref, send_sem=chain_s,
                                            recv_sem=chain_r, device_id={"sp": to}, device_id_type=MESH)

    @pl.when(sp == 0)
    def _():
        next_ref[...] = s_ref[...]
        pass_on(1).start()

    @pl.when(sp > 0)
    def _():
        pass_on(0).wait_recv()

        @pl.when(sp < nsp - 1)
        def _():
            for h in range(heads):
                next_ref[h] = s_ref[h] + dot3(split2(m_ref[h]), split2(start_ref[h]))
            pass_on(sp + 1).start()

        for h in range(heads):
            sl = slice(h * HK, (h + 1) * HK)
            o_ref[:, sl] += dot3(split2(qe_ref[:, sl]), split2(start_ref[h]))

    gain = gain_ref[...].astype(f32)
    for h in range(heads):
        sl = slice(h * HK, (h + 1) * HK)
        out = o_ref[:, sl]
        out = out * lax.rsqrt(jnp.mean(out * out, axis=1, keepdims=True) + epsilon) * gain
        mixed_ref[:, sl] = (out * jax.nn.silu(g_ref[:, sl].astype(f32))).astype(jnp.bfloat16)

    def swap(d):
        to = lax.rem(z + d, nz)
        return pltpu.make_async_remote_copy(
            src_ref=mixed_ref.at[pl.ds(to * rows, rows)], dst_ref=own_ref.at[z], send_sem=swap_s.at[d],
            recv_sem=swap_r.at[d], device_id={"tp": to}, device_id_type=MESH)

    for d in range(1, nz):
        swap(d).start()
    own_ref[z] = mixed_ref[pl.ds(z * rows, rows), :]
    experts = nsp * nz
    lanes = pay_ref.shape[1] - width
    place = lax.broadcasted_iota(jnp.int32, (lanes, rows), 0)
    table = jnp.zeros((lanes, rows), f32)
    for i in range(ids_ref.shape[0]):
        share = share_ref[i:i + 1, :]
        high = share.astype(jnp.bfloat16).astype(f32)
        chosen = ids_ref[i:i + 1, :]
        table = table + jnp.where(place == chosen, high, 0.0)
        table = table + jnp.where(place == chosen + experts, share - high, 0.0)
    eye_r = (lax.broadcasted_iota(jnp.int32, (rows, rows), 0)
             == lax.broadcasted_iota(jnp.int32, (rows, rows), 1)).astype(jnp.bfloat16)
    pay_ref[:, width:] = dot1(eye_r, table.astype(jnp.bfloat16), 1, 1).astype(jnp.bfloat16)
    load.wait()
    for d in range(1, nz):
        swap(d).wait_recv()
    flat = jnp.concatenate([own_ref[t] for t in range(nz)], axis=1)
    step = width // 4
    total = jnp.zeros((rows, 1), f32)
    for i in range(4):
        cols = slice(i * step, (i + 1) * step)
        got = (skip_ref[:, cols].astype(f32) + dot1(flat, wo[:, cols])).astype(jnp.bfloat16)
        merged_ref[:, cols] = got
        got = got.astype(f32)
        total = total + jnp.sum(got * got, axis=1, keepdims=True)
    scale = lax.rsqrt(total * (1.0 / width) + epsilon)
    for i in range(4):
        cols = slice(i * step, (i + 1) * step)
        pay_ref[:, cols] = (merged_ref[:, cols].astype(f32) * scale
                            * rescale_ref[:, cols].astype(f32)).astype(jnp.bfloat16)

    @pl.when(sp < nsp - 1)
    def _():
        pass_on(sp + 1).wait_send()

    for d in range(1, nz):
        swap(d).wait_send()


def attend(q, k, v, gate, score, added, logscale, strength_pre, gain, wo, skip, rescale, ids, shares, nz, lanes):
    heads, length = score.shape
    rows, width = skip.shape
    f32, bf = jnp.float32, jnp.bfloat16
    vm = pl.BlockSpec(memory_space=pltpu.VMEM)
    dma = pltpu.SemaphoreType.DMA
    return pl.pallas_call(
        attention_kernel,
        out_shape=(jax.ShapeDtypeStruct((rows, width + lanes), bf), jax.ShapeDtypeStruct((rows, width), bf)),
        in_specs=[vm] * 9 + [pl.BlockSpec(memory_space=pl.ANY)] + [vm] * 4,
        out_specs=(vm, vm),
        scratch_shapes=[
            pltpu.VMEM((length, heads * HK), f32),
            pltpu.VMEM((length, heads * HK), f32),
            pltpu.VMEM((heads, HK, HK), f32),
            pltpu.VMEM((heads, HK, HK), f32),
            pltpu.VMEM((heads, HK, HK), f32),
            pltpu.VMEM((heads, HK, HK), f32),
            pltpu.VMEM((length, heads * HK), bf),
            pltpu.VMEM((nz, rows, heads * HK), bf),
            pltpu.VMEM(wo.shape, bf),
            dma, dma, dma, dma((nz,)), dma((nz,)),
        ],
        compiler_params=pltpu.CompilerParams(
            collective_id=5, has_side_effects=True, vmem_limit_bytes=48 * 1024 * 1024),
        name="attend",
    )(q, k, v, gate, score, added, logscale, strength_pre, gain, wo, skip, rescale, ids, shares)


def experts_kernel(ny, nz, rows, width, experts, x_ref, merged_ref, wg_hbm, wu_hbm, wd_hbm, out_ref,
                   G, Pt, CR, YR, ZR, wg, wu, wd, wsem, own_sem,
                   zs, zr, ys, yr, cs, cr, rcs, rcr, rys, ryr, rzs, rzr):
    sp = lax.axis_index("sp")
    z = lax.axis_index("tp")
    y = sp // 2
    c = sp % 2
    pc = 1 - c
    me = sp * nz + z
    expert = me
    f32 = jnp.float32

    def slot(yy, cc, zz):
        return (yy * 2 + cc) * nz + zz

    loads = [pltpu.make_async_copy(s, d, wsem.at[i])
             for i, (s, d) in enumerate(((wg_hbm, wg), (wu_hbm, wu), (wd_hbm, wd)))]
    for load in loads:
        load.start()
    own = pltpu.make_async_copy(x_ref, G.at[me], own_sem)
    own.start()

    barrier = pltpu.get_barrier_semaphore()
    greet = [{"tp": lax.rem(z + 1, nz)}, {"tp": lax.rem(z + nz - 1, nz)},
             {"sp": lax.rem(y + 1, ny) * 2 + c}, {"sp": lax.rem(y + ny - 1, ny) * 2 + c},
             {"sp": y * 2 + pc}]
    for d in greet:
        pl.semaphore_signal(barrier, inc=1, device_id=d, device_id_type=MESH)
    pl.semaphore_wait(barrier, len(greet))

    def remote(src, dst, ssem, rsem, dev):
        return pltpu.make_async_remote_copy(src_ref=src, dst_ref=dst, send_sem=ssem, recv_sem=rsem,
                                            device_id=dev, device_id_type=MESH)

    def z_copy(d, b, src=None):
        sl = slot(y, c, b)
        return remote(G.at[sl] if src is None else src, G.at[sl], zs.at[d, b], zr.at[b],
                      {"tp": z + (1 if d == 0 else -1)})

    def y_copy(d, yy, b, src=None):
        sl = slot(yy, c, b)
        return remote(G.at[sl] if src is None else src, G.at[sl], ys.at[d, yy, b], yr.at[yy, b],
                      {"sp": (y + (1 if d == 0 else -1)) * 2 + c})

    def c_copy(yy, b, cc=None, src=None):
        cc = c if cc is None else cc
        sl = slot(yy, cc, b)
        return remote(G.at[sl] if src is None else src, G.at[sl], cs.at[yy, b], cr.at[yy, b],
                      {"sp": y * 2 + pc})

    def fan_y(b, src=None):
        @pl.when(y + 1 < ny)
        def _():
            y_copy(0, y, b, src).start()

        @pl.when(y > 0)
        def _():
            y_copy(1, y, b, src).start()

    @pl.when(z + 1 < nz)
    def _():
        z_copy(0, z, x_ref).start()

    @pl.when(z > 0)
    def _():
        z_copy(1, z, x_ref).start()

    fan_y(z, x_ref)
    c_copy(y, z, src=x_ref).start()
    own.wait()

    @pl.loop(1, nz)
    def _(s):
        for d in (0, 1):
            b = z - s if d == 0 else z + s
            ok = b >= 0 if d == 0 else b < nz
            onward = z + 1 < nz if d == 0 else z > 0

            @pl.when(ok)
            def _():
                z_copy(d, b).wait_recv()

                @pl.when(onward)
                def _():
                    z_copy(d, b).start()

                fan_y(b)
                c_copy(y, b).start()

    def compute(yy, cc):
        first = slot(yy, cc, 0)
        x = jnp.concatenate([G[first + b, :, :width] for b in range(nz)], axis=0)
        tail = jnp.concatenate([G[first + b, :, width:] for b in range(nz)], axis=0).astype(f32)
        lane = lax.broadcasted_iota(jnp.int32, tail.shape, 1)
        share = jnp.sum(jnp.where((lane == expert) | (lane == expert + experts), tail, 0.0),
                        axis=1, keepdims=True)
        gate = jnp.dot(x, wg[...], preferred_element_type=f32)
        upward = jnp.dot(x, wu[...], preferred_element_type=f32)
        hidden = (jax.nn.silu(gate) * upward).astype(jnp.bfloat16)
        half = width // 2
        for i in range(2):
            cols = slice(i * half, (i + 1) * half)
            got = (jnp.dot(hidden, wd[:, cols], preferred_element_type=f32) * share).astype(jnp.bfloat16)
            for b in range(nz):
                Pt[first + b, :, cols] = got[b * rows:(b + 1) * rows]

    for load in loads:
        load.wait()

    @pl.loop(1, ny)
    def _(t):
        for d in (0, 1):
            yy = y - t if d == 0 else y + t
            ok = yy >= 0 if d == 0 else yy < ny
            onward = y + 1 < ny if d == 0 else y > 0

            @pl.when(ok)
            def _():
                @pl.loop(0, nz)
                def _(b):
                    y_copy(d, yy, b).wait_recv()

                    @pl.when(onward)
                    def _():
                        y_copy(d, yy, b).start()

                    c_copy(yy, b).start()

    def rc_copy(yy, b):
        return remote(Pt.at[slot(yy, pc, b)], CR.at[yy, b], rcs.at[yy, b], rcr.at[yy, b],
                      {"sp": y * 2 + pc})

    @pl.loop(0, 2 * ny)
    def _(j):
        yy = lax.rem(y + lax.rem(j, ny), ny)
        cc = jnp.where(j < ny, pc, c)

        @pl.when(j < ny)
        def _():
            @pl.loop(0, nz)
            def _(b):
                c_copy(yy, b, cc=pc).wait_recv()

        compute(yy, cc)

        @pl.when(j < ny)
        def _():
            @pl.loop(0, nz)
            def _(b):
                rc_copy(yy, b).start()

    def add_to(sl, other):
        Pt[sl] = (Pt[sl].astype(f32) + other.astype(f32)).astype(jnp.bfloat16)

    def ry_copy(d, yy, b):
        dest = y + (1 if d == 0 else -1)
        place = yy if d == 0 else jnp.where(yy == dest, ny, yy)
        return remote(Pt.at[slot(yy, c, b)], YR.at[place, b], rys.at[d, yy, b], ryr.at[place, b],
                      {"sp": dest * 2 + c})

    def ry_wait(place, b):
        remote(YR.at[place, b], YR.at[place, b], rys.at[0, 0, b], ryr.at[place, b],
               {"sp": y * 2 + pc}).wait_recv()

    @pl.loop(0, ny - 1)
    def _(t):
        for d in (0, 1):
            yy = ny - 1 - t if d == 0 else t
            ok = yy > y if d == 0 else yy < y
            behind = y > 0 if d == 0 else y + 1 < ny

            @pl.when(ok)
            def _():
                @pl.loop(0, nz)
                def _(i):
                    b = jnp.where(lax.rem(i, 2) == 0, nz - 1 - i // 2, i // 2)
                    sl = slot(yy, c, b)
                    rc_copy(yy, b).wait_recv()
                    add_to(sl, CR[yy, b])

                    @pl.when(behind)
                    def _():
                        ry_wait(yy, b)
                        add_to(sl, YR[yy, b])

                    ry_copy(d, yy, b).start()

    def rz_copy(d, b):
        dest = z + (1 if d == 0 else -1)
        place = b if d == 0 else jnp.where(b == dest, nz, b)
        return remote(Pt.at[slot(y, c, b)], ZR.at[place], rzs.at[d, b], rzr.at[place], {"tp": dest})

    def rz_wait(place):
        remote(ZR.at[place], ZR.at[place], rzs.at[0, 0], rzr.at[place], {"tp": z}).wait_recv()

    @pl.loop(0, nz)
    def _(i):
        b = jnp.where(lax.rem(i, 2) == 0, nz - 1 - i // 2, i // 2)
        sl = slot(y, c, b)
        rc_copy(y, b).wait_recv()
        add_to(sl, CR[y, b])

        @pl.when(y > 0)
        def _():
            ry_wait(y, b)
            add_to(sl, YR[y, b])

        @pl.when(y + 1 < ny)
        def _():
            ry_wait(ny, b)
            add_to(sl, YR[ny, b])

        for d in (0, 1):
            ok = b > z if d == 0 else b < z
            behind = z > 0 if d == 0 else z + 1 < nz

            @pl.when(ok)
            def _():
                @pl.when(behind)
                def _():
                    rz_wait(b)
                    add_to(sl, ZR[b])

                rz_copy(d, b).start()

    @pl.when(z > 0)
    def _():
        rz_wait(z)
        add_to(me, ZR[z])

    @pl.when(z + 1 < nz)
    def _():
        rz_wait(nz)
        add_to(me, ZR[nz])

    out_ref[...] = (merged_ref[...].astype(f32) + Pt[me].astype(f32)).astype(jnp.bfloat16)

    @pl.loop(0, nz)
    def _(b):
        @pl.when((z + 1 < nz) & (b <= z))
        def _():
            z_copy(0, b).wait_send()

        @pl.when((z > 0) & (b >= z))
        def _():
            z_copy(1, b).wait_send()

        @pl.when(b > z)
        def _():
            rz_copy(0, b).wait_send()

        @pl.when(b < z)
        def _():
            rz_copy(1, b).wait_send()

        @pl.loop(0, ny)
        def _(yy):
            c_copy(yy, b).wait_send()
            rc_copy(yy, b).wait_send()

            @pl.when((y + 1 < ny) & (yy <= y))
            def _():
                y_copy(0, yy, b).wait_send()

            @pl.when((y > 0) & (yy >= y))
            def _():
                y_copy(1, yy, b).wait_send()

            @pl.when(yy > y)
            def _():
                ry_copy(0, yy, b).wait_send()

            @pl.when(yy < y)
            def _():
                ry_copy(1, yy, b).wait_send()


def run_experts(payload, merged, wg, wu, wd, ny, nz, experts):
    rows, width = merged.shape
    wide = payload.shape[1]
    hidden = wg.shape[1]
    blocks = ny * 2 * nz
    bf = jnp.bfloat16
    vm = pl.BlockSpec(memory_space=pltpu.VMEM)
    hbm = pl.BlockSpec(memory_space=pl.ANY)
    dma = pltpu.SemaphoreType.DMA
    return pl.pallas_call(
        functools.partial(experts_kernel, ny, nz, rows, width, experts),
        out_shape=jax.ShapeDtypeStruct((rows, width), bf),
        in_specs=[vm, vm, hbm, hbm, hbm],
        out_specs=vm,
        scratch_shapes=[
            pltpu.VMEM((blocks, rows, wide), bf),
            pltpu.VMEM((blocks, rows, width), bf),
            pltpu.VMEM((ny, nz, rows, width), bf),
            pltpu.VMEM((ny + 1, nz, rows, width), bf),
            pltpu.VMEM((nz + 1, rows, width), bf),
            pltpu.VMEM((width, hidden), bf),
            pltpu.VMEM((width, hidden), bf),
            pltpu.VMEM((hidden, width), bf),
            dma((3,)), dma,
            dma((2, nz)), dma((nz,)),
            dma((2, ny, nz)), dma((ny, nz)),
            dma((ny, nz)), dma((ny, nz)),
            dma((ny, nz)), dma((ny, nz)),
            dma((2, ny, nz)), dma((ny + 1, nz)),
            dma((2, nz)), dma((nz + 1,)),
        ],
        compiler_params=pltpu.CompilerParams(
            collective_id=3, has_side_effects=True, vmem_limit_bytes=VLIM),
        name="routed_experts",
    )(payload, merged, wg, wu, wd)


def local(
    attention_queryset,
    attention_keyset,
    attention_valueset,
    readout_switch_preactivation,
    retention_prelinear_score,
    additional_attenuation,
    feature_retention_logscale,
    strength_prelinear_score,
    channel_rescale_vector,
    final_projection_matrix,
    skip_stream,
    specialist_rescale_vector,
    specialist_switch_matrix,
    specialist_widen_matrix,
    specialist_contract_matrix,
    chosen_specialist_ids,
    dispatch_shares,
):
    nsp = lax.axis_size("sp")
    nz = lax.axis_size("tp")
    experts = nsp * nz
    lanes = -(-2 * experts // 128) * 128
    payload, merged = attend(
        attention_queryset,
        attention_keyset,
        attention_valueset,
        readout_switch_preactivation,
        retention_prelinear_score.T,
        additional_attenuation.T,
        feature_retention_logscale[:, None],
        strength_prelinear_score.T,
        channel_rescale_vector[None, :],
        final_projection_matrix,
        skip_stream,
        specialist_rescale_vector[None, :],
        chosen_specialist_ids.T,
        dispatch_shares.T,
        nz,
        lanes,
    )
    return run_experts(payload, merged, specialist_switch_matrix[0], specialist_widen_matrix[0],
                       specialist_contract_matrix[0], nsp // 2, nz, experts)


def solution(mesh):
    return jax.shard_map(
        local,
        mesh=mesh,
        in_specs=(
            P(("grp", "sp"), "tp"),
            P(("grp", "sp"), "tp"),
            P(("grp", "sp"), "tp"),
            P(("grp", "sp"), "tp"),
            P(("grp", "sp"), "tp"),
            P(("grp", "sp"), "tp"),
            P("tp"),
            P(("grp", "sp"), "tp"),
            P(),
            P(),
            P(("grp", "sp", "tp"), None),
            P(),
            P(("sp", "tp"), None, None),
            P(("sp", "tp"), None, None),
            P(("sp", "tp"), None, None),
            P(("grp", "sp", "tp"), None),
            P(("grp", "sp", "tp"), None),
        ),
        out_specs=P(("grp", "sp", "tp"), None),
        check_vma=False,
    )
```

```python
import functools

import jax
import jax.numpy as jnp
from jax import lax
from jax.experimental import pallas as pl
from jax.experimental.pallas import tpu as pltpu
from jax.sharding import PartitionSpec as P

HK = 128
epsilon = 1e-06
MESH = pl.DeviceIdType.MESH
VLIM = 64 * 1024 * 1024 - 128 * 1024


def split2(a):
    hi = a.astype(jnp.bfloat16)
    return hi, (a - hi.astype(jnp.float32)).astype(jnp.bfloat16)


def dims(ca, cb):
    return (((ca,), (cb,)), ((), ()))


def dot1(a, b, ca=1, cb=0):
    return lax.dot_general(a, b, dims(ca, cb), preferred_element_type=jnp.float32)


def dot3(a, b, ca=1, cb=0):
    return dot1(a[0], b[0], ca, cb) + (dot1(a[0], b[1], ca, cb) + dot1(a[1], b[0], ca, cb))


def attention_kernel(q_ref, k_ref, v_ref, g_ref, sc_ref, ad_ref, ls_ref, st_ref, gain_ref, wo_hbm, skip_ref,
                     rescale_ref, ids_ref, share_ref, pay_ref, merged_ref,
                     o_ref, qe_ref, m_ref, s_ref, start_ref, next_ref, mixed_ref, own_ref, wo,
                     wsem, chain_s, chain_r, swap_s, swap_r):
    heads, length = sc_ref.shape
    f32 = jnp.float32
    sp = lax.axis_index("sp")
    z = lax.axis_index("tp")
    nsp = lax.axis_size("sp")
    nz = lax.axis_size("tp")
    rows, width = merged_ref.shape
    load = pltpu.make_async_copy(wo_hbm, wo, wsem)
    load.start()
    barrier = pltpu.get_barrier_semaphore()
    greet = [{"sp": lax.rem(sp + 1, nsp)}, {"sp": lax.rem(sp + nsp - 1, nsp)}]
    greet += [{"tp": lax.rem(z + d, nz)} for d in range(1, nz)]
    for d in greet:
        pl.semaphore_signal(barrier, inc=1, device_id=d, device_id_type=MESH)
    row = lax.broadcasted_iota(jnp.int32, (length, length), 0)
    col = lax.broadcasted_iota(jnp.int32, (length, length), 1)
    causal = row >= col
    strict = row > col
    tri = causal.astype(jnp.float32)
    score = sc_ref[...]
    soft = jnp.maximum(score, 0.0) + jnp.log1p(jnp.exp(-jnp.abs(score)))
    ld = ad_ref[...] - jnp.exp(ls_ref[...]) * soft
    cum_col = lax.dot_general(tri, ld, dims(1, 1), precision=lax.Precision.HIGHEST,
                              preferred_element_type=jnp.float32)
    cum_row = lax.dot_general(ld, tri, dims(1, 1), precision=lax.Precision.HIGHEST,
                              preferred_element_type=jnp.float32)
    eye = (row == col).astype(jnp.float32)
    beta_all = lax.dot_general(eye, jax.nn.sigmoid(st_ref[...]), dims(1, 1), precision=lax.Precision.HIGHEST,
                               preferred_element_type=jnp.float32)
    eye_k = (lax.broadcasted_iota(jnp.int32, (HK, HK), 0)
             == lax.broadcasted_iota(jnp.int32, (HK, HK), 1)).astype(jnp.float32)
    xs, lows, keep = [], [], []
    for h in range(heads):
        sl = slice(h * HK, (h + 1) * HK)
        q = q_ref[:, sl].astype(jnp.float32)
        k = k_ref[:, sl].astype(jnp.float32)
        v = v_ref[:, sl].astype(jnp.float32)
        q = q * lax.rsqrt(jnp.sum(q * q, axis=1, keepdims=True) + epsilon) * HK ** (-0.5)
        k = k * lax.rsqrt(jnp.sum(k * k, axis=1, keepdims=True) + epsilon)
        c = cum_col[:, h:h + 1]
        r = cum_row[h:h + 1, :]
        beta = beta_all[:, h:h + 1]
        decay = jnp.where(causal, jnp.exp(jnp.minimum(c - r, 0.0)), 0.0)
        ks = split2(k)
        lower = jnp.where(strict, beta * dot3(ks, ks, 1, 1) * decay, 0.0)
        scores = split2(dot3(split2(q), ks, 1, 1) * decay)
        lows.append(lower)
        keep.append((q, k, v, c, beta, scores))
        n = jnp.where((row // 8) == (col // 8), -lower, 0.0)
        n1 = split2(n)
        n2f = dot3(n1, n1)
        n2 = split2(n2f)
        p = eye + n
        p = p + dot3(split2(p), n2)
        n4 = split2(dot3(n2, n2))
        xs.append(p + dot3(split2(p), n4))
    size = 8
    while size < length:
        mask = ((row // (2 * size)) == (col // (2 * size))) & ((row // size) != (col // size))
        for h in range(heads):
            part = split2(jnp.where(mask, lows[h], 0.0))
            x2 = split2(xs[h])
            xs[h] = xs[h] - dot3(x2, split2(dot3(part, x2)))
        size *= 2
    for h in range(heads):
        sl = slice(h * HK, (h + 1) * HK)
        q, k, v, c, beta, scores = keep[h]
        up = jnp.exp(c)
        last = c[length - 1:length, :]
        right = jnp.concatenate([v * beta, k * (beta * up)], axis=1)
        uw = split2(dot3(split2(xs[h]), split2(right)))
        mixed = dot3(scores, uw)
        o_ref[:, sl] = mixed[:, :HK]
        qe_ref[:, sl] = q * up - mixed[:, HK:]
        ends = dot3(split2(k * jnp.exp(last - c)), uw, 0, 0)
        s_ref[h] = ends[:, :HK]
        m_ref[h] = jnp.exp(last) * eye_k - ends[:, HK:]

    pl.semaphore_wait(barrier, len(greet))

    def pass_on(to):
        return pltpu.make_async_remote_copy(src_ref=next_ref, dst_ref=start_ref, send_sem=chain_s,
                                            recv_sem=chain_r, device_id={"sp": to}, device_id_type=MESH)

    @pl.when(sp == 0)
    def _():
        next_ref[...] = s_ref[...]
        pass_on(1).start()

    @pl.when(sp > 0)
    def _():
        pass_on(0).wait_recv()

        @pl.when(sp < nsp - 1)
        def _():
            for h in range(heads):
                next_ref[h] = s_ref[h] + dot3(split2(m_ref[h]), split2(start_ref[h]))
            pass_on(sp + 1).start()

        for h in range(heads):
            sl = slice(h * HK, (h + 1) * HK)
            o_ref[:, sl] += dot3(split2(qe_ref[:, sl]), split2(start_ref[h]))

    gain = gain_ref[...].astype(f32)
    for h in range(heads):
        sl = slice(h * HK, (h + 1) * HK)
        out = o_ref[:, sl]
        out = out * lax.rsqrt(jnp.mean(out * out, axis=1, keepdims=True) + epsilon) * gain
        mixed_ref[:, sl] = (out * jax.nn.silu(g_ref[:, sl].astype(f32))).astype(jnp.bfloat16)

    def swap(d):
        to = lax.rem(z + d, nz)
        return pltpu.make_async_remote_copy(
            src_ref=mixed_ref.at[pl.ds(to * rows, rows)], dst_ref=own_ref.at[z], send_sem=swap_s.at[d],
            recv_sem=swap_r.at[d], device_id={"tp": to}, device_id_type=MESH)

    for d in range(1, nz):
        swap(d).start()
    own_ref[z] = mixed_ref[pl.ds(z * rows, rows), :]
    experts = nsp * nz
    lanes = pay_ref.shape[1] - width
    place = lax.broadcasted_iota(jnp.int32, (lanes, rows), 0)
    table = jnp.zeros((lanes, rows), f32)
    for i in range(ids_ref.shape[0]):
        share = share_ref[i:i + 1, :]
        high = share.astype(jnp.bfloat16).astype(f32)
        chosen = ids_ref[i:i + 1, :]
        table = table + jnp.where(place == chosen, high, 0.0)
        table = table + jnp.where(place == chosen + experts, share - high, 0.0)
    eye_r = (lax.broadcasted_iota(jnp.int32, (rows, rows), 0)
             == lax.broadcasted_iota(jnp.int32, (rows, rows), 1)).astype(jnp.bfloat16)
    pay_ref[:, width:] = dot1(eye_r, table.astype(jnp.bfloat16), 1, 1).astype(jnp.bfloat16)
    load.wait()
    for d in range(1, nz):
        swap(d).wait_recv()
    flat = jnp.concatenate([own_ref[t] for t in range(nz)], axis=1)
    step = width // 4
    total = jnp.zeros((rows, 1), f32)
    for i in range(4):
        cols = slice(i * step, (i + 1) * step)
        got = (skip_ref[:, cols].astype(f32) + dot1(flat, wo[:, cols])).astype(jnp.bfloat16)
        merged_ref[:, cols] = got
        got = got.astype(f32)
        total = total + jnp.sum(got * got, axis=1, keepdims=True)
    scale = lax.rsqrt(total * (1.0 / width) + epsilon)
    for i in range(4):
        cols = slice(i * step, (i + 1) * step)
        pay_ref[:, cols] = (merged_ref[:, cols].astype(f32) * scale
                            * rescale_ref[:, cols].astype(f32)).astype(jnp.bfloat16)

    @pl.when(sp < nsp - 1)
    def _():
        pass_on(sp + 1).wait_send()

    for d in range(1, nz):
        swap(d).wait_send()


def fetched_kernel(count, *refs):
    sources, rest, held, sem = refs[:count], refs[count:-count], refs[-count:-1], refs[-1]
    plain = [i for i in range(count) if i != 9]
    copies = [pltpu.make_async_copy(sources[i], b, sem.at[n]) for n, (i, b) in enumerate(zip(plain, held))]
    for copy in copies:
        copy.start()
    for copy in copies:
        copy.wait()
    attention_kernel(*held[:9], sources[9], *held[9:], *rest)


def attend(q, k, v, gate, score, added, logscale, strength_pre, gain, wo, skip, rescale, ids, shares, nz, lanes):
    heads, length = score.shape
    rows, width = skip.shape
    f32, bf = jnp.float32, jnp.bfloat16
    vm = pl.BlockSpec(memory_space=pltpu.VMEM)
    dma = pltpu.SemaphoreType.DMA
    args = (q, k, v, gate, score, added, logscale, strength_pre, gain, wo, skip, rescale, ids, shares)
    return pl.pallas_call(
        functools.partial(fetched_kernel, len(args)),
        out_shape=(jax.ShapeDtypeStruct((rows, width + lanes), bf), jax.ShapeDtypeStruct((rows, width), bf)),
        in_specs=[pl.BlockSpec(memory_space=pl.ANY)] * len(args),
        out_specs=(vm, vm),
        scratch_shapes=[
            pltpu.VMEM((length, heads * HK), f32),
            pltpu.VMEM((length, heads * HK), f32),
            pltpu.VMEM((heads, HK, HK), f32),
            pltpu.VMEM((heads, HK, HK), f32),
            pltpu.VMEM((heads, HK, HK), f32),
            pltpu.VMEM((heads, HK, HK), f32),
            pltpu.VMEM((length, heads * HK), bf),
            pltpu.VMEM((nz, rows, heads * HK), bf),
            pltpu.VMEM(wo.shape, bf),
            dma, dma, dma, dma((nz,)), dma((nz,)),
            *[pltpu.VMEM(a.shape, a.dtype) for i, a in enumerate(args) if i != 9], dma((len(args) - 1,)),
        ],
        compiler_params=pltpu.CompilerParams(
            collective_id=5, has_side_effects=True, vmem_limit_bytes=VLIM),
        name="attend",
    )(*args)


def experts_kernel(ny, nz, rows, width, experts, x_ref, merged_ref, wg_hbm, wu_hbm, wd_hbm, out_ref,
                   G, Pt, CR, YR, ZR, wg, wu, wd, wsem, own_sem,
                   zs, zr, ys, yr, cs, cr, rcs, rcr, rys, ryr, rzs, rzr):
    sp = lax.axis_index("sp")
    z = lax.axis_index("tp")
    y = sp // 2
    c = sp % 2
    pc = 1 - c
    me = sp * nz + z
    expert = me
    f32 = jnp.float32

    def slot(yy, cc, zz):
        return (yy * 2 + cc) * nz + zz

    loads = [pltpu.make_async_copy(s, d, wsem.at[i])
             for i, (s, d) in enumerate(((wg_hbm, wg), (wu_hbm, wu), (wd_hbm, wd)))]
    for load in loads:
        load.start()
    own = pltpu.make_async_copy(x_ref, G.at[me], own_sem)
    own.start()

    barrier = pltpu.get_barrier_semaphore()
    greet = [{"tp": lax.rem(z + 1, nz)}, {"tp": lax.rem(z + nz - 1, nz)},
             {"sp": lax.rem(y + 1, ny) * 2 + c}, {"sp": lax.rem(y + ny - 1, ny) * 2 + c},
             {"sp": y * 2 + pc}]
    for d in greet:
        pl.semaphore_signal(barrier, inc=1, device_id=d, device_id_type=MESH)
    pl.semaphore_wait(barrier, len(greet))

    def remote(src, dst, ssem, rsem, dev):
        return pltpu.make_async_remote_copy(src_ref=src, dst_ref=dst, send_sem=ssem, recv_sem=rsem,
                                            device_id=dev, device_id_type=MESH)

    def z_copy(d, b, src=None):
        sl = slot(y, c, b)
        return remote(G.at[sl] if src is None else src, G.at[sl], zs.at[d, b], zr.at[b],
                      {"tp": z + (1 if d == 0 else -1)})

    def y_copy(d, yy, b, src=None):
        sl = slot(yy, c, b)
        return remote(G.at[sl] if src is None else src, G.at[sl], ys.at[d, yy, b], yr.at[yy, b],
                      {"sp": (y + (1 if d == 0 else -1)) * 2 + c})

    def c_copy(yy, b, cc=None, src=None):
        cc = c if cc is None else cc
        sl = slot(yy, cc, b)
        return remote(G.at[sl] if src is None else src, G.at[sl], cs.at[yy, b], cr.at[yy, b],
                      {"sp": y * 2 + pc})

    def fan_y(b, src=None):
        @pl.when(y + 1 < ny)
        def _():
            y_copy(0, y, b, src).start()

        @pl.when(y > 0)
        def _():
            y_copy(1, y, b, src).start()

    @pl.when(z + 1 < nz)
    def _():
        z_copy(0, z, x_ref).start()

    @pl.when(z > 0)
    def _():
        z_copy(1, z, x_ref).start()

    fan_y(z, x_ref)
    c_copy(y, z, src=x_ref).start()
    own.wait()

    @pl.loop(1, nz)
    def _(s):
        for d in (0, 1):
            b = z - s if d == 0 else z + s
            ok = b >= 0 if d == 0 else b < nz
            onward = z + 1 < nz if d == 0 else z > 0

            @pl.when(ok)
            def _():
                z_copy(d, b).wait_recv()

                @pl.when(onward)
                def _():
                    z_copy(d, b).start()

                fan_y(b)
                c_copy(y, b).start()

    def compute(yy, cc):
        first = slot(yy, cc, 0)
        x = jnp.concatenate([G[first + b, :, :width] for b in range(nz)], axis=0)
        tail = jnp.concatenate([G[first + b, :, width:] for b in range(nz)], axis=0).astype(f32)
        lane = lax.broadcasted_iota(jnp.int32, tail.shape, 1)
        share = jnp.sum(jnp.where((lane == expert) | (lane == expert + experts), tail, 0.0),
                        axis=1, keepdims=True)
        gate = jnp.dot(x, wg[...], preferred_element_type=f32)
        upward = jnp.dot(x, wu[...], preferred_element_type=f32)
        hidden = (jax.nn.silu(gate) * upward).astype(jnp.bfloat16)
        half = width // 2
        for i in range(2):
            cols = slice(i * half, (i + 1) * half)
            got = (jnp.dot(hidden, wd[:, cols], preferred_element_type=f32) * share).astype(jnp.bfloat16)
            for b in range(nz):
                Pt[first + b, :, cols] = got[b * rows:(b + 1) * rows]

    for load in loads:
        load.wait()

    @pl.loop(1, ny)
    def _(t):
        for d in (0, 1):
            yy = y - t if d == 0 else y + t
            ok = yy >= 0 if d == 0 else yy < ny
            onward = y + 1 < ny if d == 0 else y > 0

            @pl.when(ok)
            def _():
                @pl.loop(0, nz)
                def _(b):
                    y_copy(d, yy, b).wait_recv()

                    @pl.when(onward)
                    def _():
                        y_copy(d, yy, b).start()

                    c_copy(yy, b).start()

    def rc_copy(yy, b):
        return remote(Pt.at[slot(yy, pc, b)], CR.at[yy, b], rcs.at[yy, b], rcr.at[yy, b],
                      {"sp": y * 2 + pc})

    @pl.loop(0, 2 * ny)
    def _(j):
        yy = lax.rem(y + lax.rem(j, ny), ny)
        cc = jnp.where(j < ny, pc, c)

        @pl.when(j < ny)
        def _():
            @pl.loop(0, nz)
            def _(b):
                c_copy(yy, b, cc=pc).wait_recv()

        compute(yy, cc)

        @pl.when(j < ny)
        def _():
            @pl.loop(0, nz)
            def _(b):
                rc_copy(yy, b).start()

    def add_to(sl, other):
        Pt[sl] = (Pt[sl].astype(f32) + other.astype(f32)).astype(jnp.bfloat16)

    def ry_copy(d, yy, b):
        dest = y + (1 if d == 0 else -1)
        place = yy if d == 0 else jnp.where(yy == dest, ny, yy)
        return remote(Pt.at[slot(yy, c, b)], YR.at[place, b], rys.at[d, yy, b], ryr.at[place, b],
                      {"sp": dest * 2 + c})

    def ry_wait(place, b):
        remote(YR.at[place, b], YR.at[place, b], rys.at[0, 0, b], ryr.at[place, b],
               {"sp": y * 2 + pc}).wait_recv()

    @pl.loop(0, ny - 1)
    def _(t):
        for d in (0, 1):
            yy = ny - 1 - t if d == 0 else t
            ok = yy > y if d == 0 else yy < y
            behind = y > 0 if d == 0 else y + 1 < ny

            @pl.when(ok)
            def _():
                @pl.loop(0, nz)
                def _(i):
                    b = jnp.where(lax.rem(i, 2) == 0, nz - 1 - i // 2, i // 2)
                    sl = slot(yy, c, b)
                    rc_copy(yy, b).wait_recv()
                    add_to(sl, CR[yy, b])

                    @pl.when(behind)
                    def _():
                        ry_wait(yy, b)
                        add_to(sl, YR[yy, b])

                    ry_copy(d, yy, b).start()

    def rz_copy(d, b):
        dest = z + (1 if d == 0 else -1)
        place = b if d == 0 else jnp.where(b == dest, nz, b)
        return remote(Pt.at[slot(y, c, b)], ZR.at[place], rzs.at[d, b], rzr.at[place], {"tp": dest})

    def rz_wait(place):
        remote(ZR.at[place], ZR.at[place], rzs.at[0, 0], rzr.at[place], {"tp": z}).wait_recv()

    @pl.loop(0, nz)
    def _(i):
        b = jnp.where(lax.rem(i, 2) == 0, nz - 1 - i // 2, i // 2)
        sl = slot(y, c, b)
        rc_copy(y, b).wait_recv()
        add_to(sl, CR[y, b])

        @pl.when(y > 0)
        def _():
            ry_wait(y, b)
            add_to(sl, YR[y, b])

        @pl.when(y + 1 < ny)
        def _():
            ry_wait(ny, b)
            add_to(sl, YR[ny, b])

        for d in (0, 1):
            ok = b > z if d == 0 else b < z
            behind = z > 0 if d == 0 else z + 1 < nz

            @pl.when(ok)
            def _():
                @pl.when(behind)
                def _():
                    rz_wait(b)
                    add_to(sl, ZR[b])

                rz_copy(d, b).start()

    @pl.when(z > 0)
    def _():
        rz_wait(z)
        add_to(me, ZR[z])

    @pl.when(z + 1 < nz)
    def _():
        rz_wait(nz)
        add_to(me, ZR[nz])

    out_ref[...] = (merged_ref[...].astype(f32) + Pt[me].astype(f32)).astype(jnp.bfloat16)

    @pl.loop(0, nz)
    def _(b):
        @pl.when((z + 1 < nz) & (b <= z))
        def _():
            z_copy(0, b).wait_send()

        @pl.when((z > 0) & (b >= z))
        def _():
            z_copy(1, b).wait_send()

        @pl.when(b > z)
        def _():
            rz_copy(0, b).wait_send()

        @pl.when(b < z)
        def _():
            rz_copy(1, b).wait_send()

        @pl.loop(0, ny)
        def _(yy):
            c_copy(yy, b).wait_send()
            rc_copy(yy, b).wait_send()

            @pl.when((y + 1 < ny) & (yy <= y))
            def _():
                y_copy(0, yy, b).wait_send()

            @pl.when((y > 0) & (yy >= y))
            def _():
                y_copy(1, yy, b).wait_send()

            @pl.when(yy > y)
            def _():
                ry_copy(0, yy, b).wait_send()

            @pl.when(yy < y)
            def _():
                ry_copy(1, yy, b).wait_send()


def run_experts(payload, merged, wg, wu, wd, ny, nz, experts):
    rows, width = merged.shape
    wide = payload.shape[1]
    hidden = wg.shape[1]
    blocks = ny * 2 * nz
    bf = jnp.bfloat16
    vm = pl.BlockSpec(memory_space=pltpu.VMEM)
    hbm = pl.BlockSpec(memory_space=pl.ANY)
    dma = pltpu.SemaphoreType.DMA
    return pl.pallas_call(
        functools.partial(experts_kernel, ny, nz, rows, width, experts),
        out_shape=jax.ShapeDtypeStruct((rows, width), bf),
        in_specs=[vm, vm, hbm, hbm, hbm],
        out_specs=vm,
        scratch_shapes=[
            pltpu.VMEM((blocks, rows, wide), bf),
            pltpu.VMEM((blocks, rows, width), bf),
            pltpu.VMEM((ny, nz, rows, width), bf),
            pltpu.VMEM((ny + 1, nz, rows, width), bf),
            pltpu.VMEM((nz + 1, rows, width), bf),
            pltpu.VMEM((width, hidden), bf),
            pltpu.VMEM((width, hidden), bf),
            pltpu.VMEM((hidden, width), bf),
            dma((3,)), dma,
            dma((2, nz)), dma((nz,)),
            dma((2, ny, nz)), dma((ny, nz)),
            dma((ny, nz)), dma((ny, nz)),
            dma((ny, nz)), dma((ny, nz)),
            dma((2, ny, nz)), dma((ny + 1, nz)),
            dma((2, nz)), dma((nz + 1,)),
        ],
        compiler_params=pltpu.CompilerParams(
            collective_id=3, has_side_effects=True, vmem_limit_bytes=VLIM),
        name="routed_experts",
    )(payload, merged, wg, wu, wd)


def local(
    attention_queryset,
    attention_keyset,
    attention_valueset,
    readout_switch_preactivation,
    retention_prelinear_score,
    additional_attenuation,
    feature_retention_logscale,
    strength_prelinear_score,
    channel_rescale_vector,
    final_projection_matrix,
    skip_stream,
    specialist_rescale_vector,
    specialist_switch_matrix,
    specialist_widen_matrix,
    specialist_contract_matrix,
    chosen_specialist_ids,
    dispatch_shares,
):
    nsp = lax.axis_size("sp")
    nz = lax.axis_size("tp")
    experts = nsp * nz
    lanes = -(-2 * experts // 128) * 128
    payload, merged = attend(
        attention_queryset,
        attention_keyset,
        attention_valueset,
        readout_switch_preactivation,
        retention_prelinear_score.T,
        additional_attenuation.T,
        feature_retention_logscale[:, None],
        strength_prelinear_score.T,
        channel_rescale_vector[None, :],
        final_projection_matrix,
        skip_stream,
        specialist_rescale_vector[None, :],
        chosen_specialist_ids.T,
        dispatch_shares.T,
        nz,
        lanes,
    )
    return run_experts(payload, merged, specialist_switch_matrix[0], specialist_widen_matrix[0],
                       specialist_contract_matrix[0], nsp // 2, nz, experts)


def solution(mesh):
    return jax.shard_map(
        local,
        mesh=mesh,
        in_specs=(
            P(("grp", "sp"), "tp"),
            P(("grp", "sp"), "tp"),
            P(("grp", "sp"), "tp"),
            P(("grp", "sp"), "tp"),
            P(("grp", "sp"), "tp"),
            P(("grp", "sp"), "tp"),
            P("tp"),
            P(("grp", "sp"), "tp"),
            P(),
            P(),
            P(("grp", "sp", "tp"), None),
            P(),
            P(("sp", "tp"), None, None),
            P(("sp", "tp"), None, None),
            P(("sp", "tp"), None, None),
            P(("grp", "sp", "tp"), None),
            P(("grp", "sp", "tp"), None),
        ),
        out_specs=P(("grp", "sp", "tp"), None),
        check_vma=False,
    )
```
